32 devices in a mesh: kv: 8 (over z, y), tp: 4 (over x, core).
Axes of the slice: x: 2, y: 2, z: 4, core: 2. Of those that a mesh axis runs over, the one named last changes fastest.
Arguments:
- hidden: bfloat16 [128, 4096], P(None, 'tp'), may hold values from -50 to 50
- input_gain: bfloat16 [4096], P('tp'), may hold values from 0.099609375 to 1.8984375
- x_weight: bfloat16 [4096, 8192], P('tp', 'kv'), may hold values from -0.09375 to 0.09375
- z_weight: bfloat16 [4096, 8192], P('tp', 'kv'), may hold values from -0.09375 to 0.09375
- bc_weight: bfloat16 [4096, 8192], P('tp', 'kv'), may hold values from -0.09375 to 0.09375
- dt_weight: bfloat16 [4096, 128], P('tp', 'kv'), may hold values from -0.09375 to 0.09375
- x_kernel: bfloat16 [4, 8192], P(None, 'kv'), may hold values from -3 to 3
- bc_kernel: bfloat16 [4, 8192], P(None, 'kv'), may hold values from -3 to 3
- dt_bias: float32 [128], P('kv'), may hold values from -3 to 0.5
- decay_log: float32 [128], P('kv'), may hold values from -3 to 1.5
- skip_scale: float32 [128], P('kv'), may hold values from 0.5 to 1.5
- output_gain: bfloat16 [8192], P('kv'), may hold values from 0.099609375 to 1.8984375
- output_weight: bfloat16 [8192, 4096], P('kv'), may hold values from -0.09375 to 0.09375
- saved_states: float32 [32, 5, 128, 64, 128], P('tp', None, 'kv'), may hold values from -1.8 to 1.8
- x_history: bfloat16 [32, 7, 8192], P('tp', None, 'kv'), may hold values from -6 to 6
- bc_history: bfloat16 [32, 7, 8192], P('tp', None, 'kv'), may hold values from -6 to 6
- accepted: int32 [32], P('tp'), may hold values from 0 to 4
Outputs:
- mixed: bfloat16 [128, 4096], P('tp', 'kv')
- new_states: float32 [32, 5, 128, 64, 128], P('tp', None, 'kv')
- x_window: bfloat16 [32, 7, 8192], P('tp', None, 'kv')
- bc_window: bfloat16 [32, 7, 8192], P('tp', None, 'kv')
The draws below stay inside these ranges and needn't reach their ends.
All inputs are finite; a program needn't handle non-finite values.
Results may differ from the reference program's by a relative error of at most 0.02.
Values may be sent and summed in bfloat16 or wider, within the bound.
A program may use at most 192 MiB of HBM per device.

```python
import jax
import jax.numpy as jnp
from jax import lax

D = 4096
HEADS = 128
HEAD_SIZE = 64
STATE = 128
GROUPS = 32
CONV = 4
PROPS = 4
SEQS = 32
TOKENS = 128
INNER = 8192
BC_WIDTH = 8192
HIST = 7
FEATURE_BLOCKS = 4


def draw_hidden(key, part):
    noise_key = jax.random.fold_in(key, 0)
    samples = jnp.clip(jax.random.normal(noise_key, (TOKENS, D), jnp.float32), -6.0, 6.0)
    quarter = jnp.arange(D) * 4 // D
    factors = jnp.array([0.5, 1.6, 0.4, 1.2], jnp.float32)[quarter]
    return (samples * factors[None, :]).astype(jnp.bfloat16)


def set_ends(result, rng, smallest, top_value):
    longest = result.shape.index(max(result.shape))
    spots = []
    for shift in (0, 1):
        where = [jax.random.randint(jax.random.fold_in(rng, axis), (), 0, length) for axis, length in enumerate(result.shape)]
        where[longest] = (where[longest] + shift) % result.shape[longest]
        spots.append(tuple(where))
    return result.at[spots[0]].set(smallest).at[spots[1]].set(top_value)


def with_spikes(entries, rng, source, target, shards_of, factor):
    owner, partner = [(jnp.arange(entries.shape[dim]) // (entries.shape[dim] // shards_of)).reshape([-1 if axis == dim else 1 for axis in range(entries.ndim)]) for dim in (source, target)]
    chosen = jax.random.permutation(rng, shards_of)[partner]
    strong = (owner == chosen) | (owner == (partner + shards_of // 2) % shards_of)
    return jnp.where(strong, factor * entries, entries)


def level_of(rng, extent, shards, low, top_value):
    gain = 1.0
    for axis_at, blocks in shards:
        draws = jax.random.uniform(jax.random.fold_in(jax.random.fold_in(rng, 6), axis_at), (blocks,), jnp.float32, low / len(shards), top_value / len(shards))
        gain = gain * jnp.repeat(jnp.exp(draws), extent[axis_at] // blocks).reshape((-1,) + (1,) * (len(extent) - 1 - axis_at))
    return gain


def bell_draw(key, dims, width, limit, cuts=(), kind=jnp.bfloat16):
    gain = level_of(key, dims, cuts, -0.22, 0.18) if cuts else 1.0
    values = jax.random.normal(key, dims, jnp.float32) * width * gain
    return jnp.minimum(jnp.maximum(values, -limit), limit).astype(kind)


def noise_with(stream_key, extent, spread, reach, cuts, heavy, kind=jnp.bfloat16):
    result = spread * jax.random.normal(stream_key, extent, jnp.float32)
    if cuts:
        result = result * level_of(stream_key, extent, cuts, -0.22, 0.18)
    return jnp.clip(with_spikes(result, jax.random.fold_in(stream_key, 3), *heavy), -reach, reach).astype(kind)


def setup_inputs(seed: int = 0) -> dict:
    streams_of = jax.random.split(jax.random.key(seed), 18)
    return {
        "hidden": draw_hidden(jax.random.fold_in(streams_of[17], 71), 0),
        "input_gain": jnp.clip(1.0 + 0.18 * jax.random.normal(streams_of[1], (D,), jnp.float32), 0.099609375, 1.8984375).astype(jnp.bfloat16),
        "x_weight": bell_draw(streams_of[2], (D, INNER), D ** -0.5, 0.09375, ((0, 4), (1, 8))),
        "z_weight": bell_draw(streams_of[3], (D, INNER), D ** -0.5, 0.09375, ((0, 4), (1, 8))),
        "bc_weight": bell_draw(streams_of[4], (D, BC_WIDTH), D ** -0.5, 0.09375, ((0, 4), (1, 8))),
        "dt_weight": bell_draw(streams_of[5], (D, HEADS), D ** -0.5, 0.09375, ((0, 4), (1, 8))),
        "x_kernel": bell_draw(streams_of[6], (CONV, INNER), CONV ** -0.5, 3.0, ((1, 8),)),
        "bc_kernel": bell_draw(streams_of[7], (CONV, BC_WIDTH), CONV ** -0.5, 3.0, ((1, 8),)),
        "dt_bias": jnp.clip(-3.0 + 3.5 * jax.random.uniform(streams_of[8], (HEADS,), jnp.float32) ** level_of(streams_of[8], (HEADS,), ((0, 8),), -0.2, 0.2), -3.0, 0.5),
        "decay_log": jnp.clip(-3.0 + 4.5 * jax.random.uniform(streams_of[9], (HEADS,), jnp.float32) ** level_of(streams_of[9], (HEADS,), ((0, 8),), -0.2, 0.2), -3.0, 1.5),
        "skip_scale": jnp.clip(0.5 + 1.0 * jax.random.uniform(streams_of[10], (HEADS,), jnp.float32) ** level_of(streams_of[10], (HEADS,), ((0, 8),), -0.2, 0.2), 0.5, 1.5),
        "output_gain": jnp.clip(1.0 + 0.18 * jax.random.normal(streams_of[11], (INNER,), jnp.float32), 0.099609375, 1.8984375).astype(jnp.bfloat16),
        "output_weight": noise_with(streams_of[12], (INNER, D), INNER ** -0.5, 0.09375, ((0, 8),), (0, 1, 8, 2.0)),
        "saved_states": bell_draw(streams_of[13], (SEQS, PROPS + 1, HEADS, HEAD_SIZE, STATE), 0.3, 1.8, ((0, 4), (2, 8)), jnp.float32),
        "x_history": bell_draw(streams_of[14], (SEQS, HIST, INNER), 1.0, 6.0, ((0, 4), (2, 8))),
        "bc_history": bell_draw(streams_of[15], (SEQS, HIST, BC_WIDTH), 1.0, 6.0, ((0, 4), (2, 8))),
        "accepted": set_ends(jax.random.randint(streams_of[16], (SEQS,), 0, PROPS + 1), jax.random.fold_in(streams_of[16], 1), 0, PROPS).astype(jnp.int32),
    }


EPSILON = 1e-05

def take_window(history, accepted, fresh_rows):
    history_len = history.shape[1] - fresh_rows.shape[1]
    indices = accepted[:, None] + jnp.arange(history_len, dtype=jnp.int32)[None, :]
    kept_rows = jnp.take_along_axis(history, indices[:, :, None], axis=1)
    return jnp.concatenate([kept_rows, fresh_rows], axis=1)

def conv_silu(window, kernel):
    length = window.shape[1] - kernel.shape[0] + 1
    running = window[:, 0:length].astype(jnp.float32) * kernel[0].astype(jnp.float32)
    for offset in range(1, kernel.shape[0]):
        running = running + window[:, offset:offset + length].astype(jnp.float32) * kernel[offset].astype(jnp.float32)
    return jax.nn.silu(running)

def ssd_block(x_conv, step_size, decay_rate, b_terms, c_terms, first_state, skip_scale):
    cumulated = jnp.cumsum(-decay_rate * step_size, axis=1)
    length = x_conv.shape[1]
    indices = jnp.arange(length)
    causal = indices[:, None] >= indices[None, :]
    gaps = cumulated[:, :, None, :] - cumulated[:, None, :, :]
    weights = jnp.exp(jnp.where(causal[None, :, :, None], gaps, -jnp.inf))
    inputs = x_conv * step_size[..., None]
    outer_prod = jnp.einsum('srhp,srhn->srhpn', inputs, b_terms)
    states = jnp.exp(cumulated)[..., None, None] * first_state[:, None] + jnp.einsum('strh,srhpn->sthpn', weights, outer_prod)
    output = jnp.einsum('sthn,sthpn->sthp', c_terms, states) + skip_scale[:, None] * x_conv
    return (output, states)

def reference(hidden, input_gain, x_weight, z_weight, bc_weight, dt_weight, x_kernel, bc_kernel, dt_bias, decay_log, skip_scale, output_gain, output_weight, saved_states, x_history, bc_history, accepted):
    widened = hidden.astype(jnp.float32)
    normed = (widened * lax.rsqrt(lax.optimization_barrier(jnp.mean(widened * widened, axis=1, keepdims=True)) + EPSILON) * input_gain.astype(jnp.float32)).astype(jnp.bfloat16)
    weights = jnp.concatenate([x_weight, z_weight, bc_weight, dt_weight], axis=1)
    feature_block = D // FEATURE_BLOCKS
    running = jnp.zeros((normed.shape[0], weights.shape[1]), jnp.float32)
    for part_index in range(FEATURE_BLOCKS):
        product = jnp.dot(normed[:, part_index * feature_block:(part_index + 1) * feature_block], weights[part_index * feature_block:(part_index + 1) * feature_block], preferred_element_type=jnp.float32)
        running = running + lax.optimization_barrier(product.astype(jnp.bfloat16)).astype(jnp.float32)
    projected = running.astype(jnp.bfloat16)
    x_fresh = projected[:, :INNER]
    z_fresh = projected[:, INNER:2 * INNER]
    bc_fresh = projected[:, 2 * INNER:2 * INNER + BC_WIDTH]
    dt_fresh = projected[:, 2 * INNER + BC_WIDTH:]
    x_window = take_window(x_history, accepted, x_fresh.reshape(SEQS, PROPS, INNER))
    bc_window = take_window(bc_history, accepted, bc_fresh.reshape(SEQS, PROPS, BC_WIDTH))
    x_conv = conv_silu(x_window, x_kernel).reshape(SEQS, PROPS, HEADS, HEAD_SIZE)
    bc_conv = conv_silu(bc_window, bc_kernel).reshape(SEQS, PROPS, GROUPS, 2, STATE)
    b_terms = jnp.repeat(bc_conv[:, :, :, 0], HEADS // GROUPS, axis=2)
    c_terms = jnp.repeat(bc_conv[:, :, :, 1], HEADS // GROUPS, axis=2)
    step_size = jax.nn.softplus(dt_fresh.astype(jnp.float32).reshape(SEQS, PROPS, HEADS) + dt_bias)
    first_state = jnp.take_along_axis(saved_states, accepted[:, None, None, None, None], axis=1)[:, 0]
    decay_rate = jnp.exp(decay_log)

    def one_sequence(pieces):
        x_one, step_one, b_one, c_one, state_one = pieces
        out_one, states_one = ssd_block(x_one[None], step_one[None], decay_rate, b_one[None], c_one[None], state_one[None], skip_scale)
        return (out_one[0], states_one[0])
    output, states = lax.map(one_sequence, (x_conv, step_size, b_terms, c_terms, first_state))
    new_states = jnp.concatenate([first_state[:, None], states], axis=1)
    gate_values = z_fresh.astype(jnp.float32).reshape(SEQS, PROPS, HEADS, HEAD_SIZE)
    gated = (output * jax.nn.silu(gate_values)).reshape(TOKENS, INNER)
    scaled = (gated * output_gain.astype(jnp.float32)).astype(jnp.bfloat16)
    branch = jnp.dot(scaled, output_weight, preferred_element_type=jnp.float32)
    mixed = (lax.rsqrt(lax.optimization_barrier(jnp.mean(gated * gated, axis=1)) + EPSILON)[:, None] * branch).astype(jnp.bfloat16)
    return (mixed, new_states, x_window, bc_window)
```

```python
import jax
import jax.numpy as jnp
import functools

from jax import lax
from jax.experimental import pallas as pl
from jax.experimental.pallas import tpu as pltpu
from jax.sharding import PartitionSpec as P

D = 4096
PROPS = 4
INNER = 8192


EPSILON = 1e-05


def partner_2(block, axis, stride):
    count = lax.axis_size(axis)
    route = []
    for low in range(count):
        high = low | 1 << stride
        if high != low and high < count:
            route += [(low, high), (high, low)]
    return lax.ppermute(block, axis, route)


def take_window(history, accepted, fresh_rows):
    history_len = history.shape[1] - fresh_rows.shape[1]
    indices = accepted[:, None] + jnp.arange(history_len, dtype=jnp.int32)[None, :]
    kept_rows = jnp.take_along_axis(history, indices[:, :, None], axis=1)
    return jnp.concatenate([kept_rows, fresh_rows], axis=1)


def conv_silu(window, kernel):
    length = window.shape[1] - kernel.shape[0] + 1
    running = window[:, 0:length].astype(jnp.float32) * kernel[0].astype(jnp.float32)
    for offset in range(1, kernel.shape[0]):
        running = running + window[:, offset : offset + length].astype(jnp.float32) * kernel[
            offset
        ].astype(jnp.float32)
    return jax.nn.silu(running)


def ssd_block(x_conv, step_size, decay_rate, b_terms, c_terms, first_state, skip_scale):
    cumulated = jnp.cumsum(-decay_rate * step_size, axis=1)
    length = x_conv.shape[1]
    indices = jnp.arange(length)
    causal = indices[:, None] >= indices[None, :]
    gaps = cumulated[:, :, None, :] - cumulated[:, None, :, :]
    weights = jnp.exp(jnp.where(causal[None, :, :, None], gaps, -jnp.inf))
    inputs = x_conv * step_size[..., None]
    outer_prod = jnp.einsum("srhp,srhn->srhpn", inputs, b_terms)
    states = jnp.exp(cumulated)[..., None, None] * first_state[:, None] + jnp.einsum(
        "strh,srhpn->sthpn", weights, outer_prod
    )
    output = jnp.einsum("sthn,sthpn->sthp", c_terms, states) + skip_scale[:, None] * x_conv
    return (output, states)


def local_general(
    hidden,
    input_gain,
    x_weight,
    z_weight,
    bc_weight,
    dt_weight,
    x_kernel,
    bc_kernel,
    dt_bias,
    decay_log,
    skip_scale,
    output_gain,
    output_weight,
    saved_states,
    x_history,
    bc_history,
    accepted,
):
    heads_here = dt_bias.shape[0]
    head_size = x_weight.shape[1] // heads_here
    state_size = saved_states.shape[4]
    seqs_here = accepted.shape[0]
    rows_here = hidden.shape[0] // lax.axis_size("tp")
    inner_here = x_weight.shape[1]
    bc_here = bc_weight.shape[1]
    widened = hidden.astype(jnp.float32)
    squares = lax.psum(jnp.sum(widened * widened, axis=1), "tp")
    normed = (
        widened * lax.rsqrt(squares[:, None] / D + EPSILON) * input_gain.astype(jnp.float32)
    ).astype(jnp.bfloat16)
    weights = jnp.concatenate([x_weight, z_weight, bc_weight, dt_weight], axis=1)
    product = jnp.dot(normed, weights, preferred_element_type=jnp.float32)
    projected = lax.psum_scatter(
        lax.optimization_barrier(product.astype(jnp.bfloat16))
        .astype(jnp.float32)
        .astype(jnp.bfloat16),
        "tp",
        scatter_dimension=0,
        tiled=True,
    )
    x_fresh = projected[:, :inner_here]
    z_fresh = projected[:, inner_here : 2 * inner_here]
    bc_fresh = projected[:, 2 * inner_here : 2 * inner_here + bc_here]
    dt_fresh = projected[:, 2 * inner_here + bc_here :]
    x_window = take_window(x_history, accepted, x_fresh.reshape(seqs_here, PROPS, inner_here))
    bc_window = take_window(bc_history, accepted, bc_fresh.reshape(seqs_here, PROPS, bc_here))
    x_conv = conv_silu(x_window, x_kernel).reshape(seqs_here, PROPS, heads_here, head_size)
    bc_conv = conv_silu(bc_window, bc_kernel)
    spread = max(4 // heads_here, 1)
    position = lax.axis_index("kv")
    for level in range(spread.bit_length() - 1):
        partner = partner_2(bc_conv, "kv", level)
        low_half = position // 2**level % 2 == 0
        bc_conv = jnp.where(
            low_half,
            jnp.concatenate([bc_conv, partner], axis=2),
            jnp.concatenate([partner, bc_conv], axis=2),
        )
    groups_here = bc_conv.shape[2] // (2 * state_size)
    paired = bc_conv.reshape(seqs_here, PROPS, groups_here, 2, state_size)
    per_group = heads_here // groups_here
    b_terms = jnp.repeat(paired[:, :, :, 0], per_group, axis=2)
    c_terms = jnp.repeat(paired[:, :, :, 1], per_group, axis=2)
    step_size = jax.nn.softplus(
        dt_fresh.astype(jnp.float32).reshape(seqs_here, PROPS, heads_here) + dt_bias
    )
    first_state = jnp.take_along_axis(saved_states, accepted[:, None, None, None, None], axis=1)[
        :, 0
    ]
    output, states = ssd_block(
        x_conv, step_size, jnp.exp(decay_log), b_terms, c_terms, first_state, skip_scale
    )
    new_states = jnp.concatenate([first_state[:, None], states], axis=1)
    gate_values = z_fresh.astype(jnp.float32).reshape(seqs_here, PROPS, heads_here, head_size)
    gated = (output * jax.nn.silu(gate_values)).reshape(rows_here, inner_here)
    square_sum = jnp.sum(gated * gated, axis=1)
    scaled = (gated * output_gain.astype(jnp.float32)).astype(jnp.bfloat16)
    partial_value = jnp.dot(scaled, output_weight, preferred_element_type=jnp.float32)
    total_squares = lax.psum(square_sum, "kv")
    summed = lax.psum_scatter(partial_value, "kv", scatter_dimension=1, tiled=True)
    mixed = (lax.rsqrt(total_squares / INNER + EPSILON)[:, None] * summed).astype(jnp.bfloat16)
    return (mixed, new_states, x_window, bc_window)


NN = (((1,), (0,)), ((), ()))
NT = (((1,), (1,)), ((), ()))
TN = (((0,), (0,)), ((), ()))


def dot(a, b, dims=NN, **kw):
    return lax.dot_general(a, b, dims, preferred_element_type=jnp.float32, **kw)


def silu(v):
    return v / (1.0 + jnp.exp(-v))


def softplus(v):
    return jnp.maximum(v, 0.0) + jnp.log(1.0 + jnp.exp(-jnp.abs(v)))


def mix_kernel(
    features, channels, n_out,
    acc_smem, acc_ref, proj_ref, xh_ref, bch_ref, xk_ref, bck_ref, par_ref, gain_ref,
    saved_ref, w_ref,
    part_ref, xw_ref, bcw_ref, xdt_ref, b_ref, a_ref,
    s0_buf, w_buf, s0_sem, w_sem,
):
    seqs = acc_smem.shape[0]
    props = proj_ref.shape[0] // seqs
    rows = seqs * props
    inner = xh_ref.shape[2]
    bcw = bch_ref.shape[2]
    heads, size, state = s0_buf.shape[1:]
    groups = bcw // (2 * state)
    per = heads // groups
    span = per * size

    def s0_copy(s):
        return pltpu.make_async_copy(
            saved_ref.at[s, acc_smem[s]], s0_buf.at[s], s0_sem.at[s])

    for s in range(seqs):
        s0_copy(s).start()
    block = w_ref.shape[1] // n_out
    w_copies = [
        pltpu.make_async_copy(
            w_ref.at[:, pl.ds(i * block, block)], w_buf.at[i], w_sem.at[i])
        for i in range(n_out)
    ]
    for copy in w_copies:
        copy.start()

    ri = lax.broadcasted_iota(jnp.int32, (rows, rows), 0)
    ci = lax.broadcasted_iota(jnp.int32, (rows, rows), 1)
    to_steps = ((ri % seqs) * props + ri // seqs == ci).astype(jnp.float32).astype(jnp.bfloat16)
    back = ((ci % seqs) * props + ci // seqs == ri).astype(jnp.float32).astype(jnp.bfloat16)

    dt_at = 2 * inner + bcw
    last = proj_ref.shape[1]
    squares = proj_ref[:, last - 128 :].astype(jnp.float32)[:, 127:128]
    scale = lax.rsqrt(squares / features + EPSILON)

    def fresh(lo, hi):
        v = (proj_ref[:, lo:hi].astype(jnp.float32) * scale).astype(jnp.bfloat16)
        return dot(to_steps, v)

    def step(v, t):
        return v[t * seqs : (t + 1) * seqs]

    acc = acc_ref[...]

    def window(hist_ref, rows_fresh, out_ref):
        kept = hist_ref.shape[0] - props
        hist = [hist_ref[m].astype(jnp.float32) for m in range(hist_ref.shape[0])]
        win = []
        for k in range(kept):
            v = hist[k]
            for j in range(1, props + 1):
                v = jnp.where(acc == j, hist[j + k], v)
            win.append(v)
        win += [step(rows_fresh, t) for t in range(props)]
        for m, v in enumerate(win):
            out_ref[m] = v.astype(jnp.bfloat16)
        return win

    def conv(win, kernel_ref):
        taps = [kernel_ref[j : j + 1].astype(jnp.float32) for j in range(kernel_ref.shape[0])]
        out = []
        for t in range(props):
            v = win[t] * taps[0]
            for j in range(1, len(taps)):
                v = v + win[t + j] * taps[j]
            out.append(silu(v))
        return out

    bc = conv(window(bch_ref, fresh(2 * inner, dt_at), bcw_ref), bck_ref)
    b_all = jnp.concatenate(
        [jnp.concatenate([v[:, 2 * g * state : (2 * g + 1) * state] for g in range(groups)], axis=1) for v in bc], axis=0)
    c_all = jnp.concatenate(
        [jnp.concatenate([v[:, (2 * g + 1) * state : (2 * g + 2) * state] for g in range(groups)], axis=1) for v in bc], axis=0)
    b_ref[...] = b_all.astype(jnp.bfloat16)
    c_low = c_all.astype(jnp.bfloat16)
    xc = conv(window(xh_ref, fresh(0, inner), xw_ref), xk_ref)

    dt_raw = fresh(dt_at, last)
    eh = lax.broadcasted_iota(jnp.int32, (128, inner), 0)
    ec = lax.broadcasted_iota(jnp.int32, (128, inner), 1)
    expand = (eh == ec // size).astype(jnp.float32)
    par = par_ref[...]
    wide = dot(par, expand, precision=lax.Precision.HIGHEST)
    dtw = dot(dt_raw.astype(jnp.bfloat16), expand.astype(jnp.bfloat16))
    lane = lax.broadcasted_iota(jnp.int32, (rows, 128), 1)
    raw = jnp.where(lane < heads, dt_raw, 0.0)
    a_ref[...] = jnp.exp(-jnp.exp(par[1:2]) * softplus(raw + par[0:1]))
    bias, rate, skip = wide[0:1], jnp.exp(wide[1:2]), wide[2:3]
    sizes = [softplus(step(dtw, t) + bias) for t in range(props)]
    xdt = [xc[t] * sizes[t] for t in range(props)]
    xdt_ref[...] = jnp.concatenate(xdt, axis=0).astype(jnp.bfloat16)

    row = lax.broadcasted_iota(jnp.int32, (rows, span), 0)
    carried = [jnp.zeros((rows, span), jnp.float32) for _ in range(groups)]
    for s in range(seqs):
        s0_copy(s).wait()
        for g in range(groups):
            s0 = s0_buf[s, g * per : (g + 1) * per].reshape(span, state).astype(jnp.bfloat16)
            got = dot(c_low[:, g * state : (g + 1) * state], s0, NT)
            carried[g] = jnp.where(row % seqs == s, got, carried[g])
    carried = jnp.concatenate(carried, axis=1)

    decays = [-rate * v for v in sizes]
    gated, sums = [], []
    zs = fresh(inner, 2 * inner)
    gain = gain_ref[...].astype(jnp.float32)
    for t in range(props):
        total = decays[t]
        out = skip * xc[t]
        ct = step(c_all, t)
        for r in range(t, -1, -1):
            br = step(b_all, r)
            prod = ct * br
            pair = jnp.concatenate(
                [jnp.broadcast_to(
                    jnp.sum(prod[:, g * state : (g + 1) * state], axis=1, keepdims=True),
                    (seqs, span)) for g in range(groups)], axis=1)
            if r == t:
                out = out + pair * xdt[r]
            else:
                out = out + jnp.exp(total) * pair * xdt[r]
                total = total + decays[r]
        out = out + jnp.exp(total) * step(carried, t)
        v = out * silu(step(zs, t))
        gated.append((v * gain).astype(jnp.bfloat16))
        sums.append(jnp.broadcast_to(jnp.sum(v * v, axis=1, keepdims=True), (seqs, 128)))
    scaled = dot(back, jnp.concatenate(gated, axis=0)).astype(jnp.bfloat16)
    sums = jnp.concatenate(sums, axis=0)
    high = sums.astype(jnp.bfloat16)
    low = (sums - high.astype(jnp.float32)).astype(jnp.bfloat16)
    sums = dot(back, high) + dot(back, low)
    for i in range(n_out):
        w_copies[i].wait()
        part_ref[i, :, :block] = dot(scaled, w_buf[i]).astype(part_ref.dtype)
        part_ref[i, :, block:] = sums.astype(part_ref.dtype)


def state_kernel(acc_smem, a_smem, xdt_ref, b_ref, s0_ref, out_ref):
    s = pl.program_id(0)
    seqs = acc_smem.shape[0]
    rows = xdt_ref.shape[0]
    props = rows // seqs
    heads, size, state = s0_ref.shape[2:]
    groups = b_ref.shape[1] // state
    per = heads // groups
    row = lax.broadcasted_iota(jnp.int32, (rows, state), 0)
    first = s0_ref[0, 0]
    out_ref[0, 0] = first
    for g in range(groups):
        b = b_ref[:, g * state : (g + 1) * state].astype(jnp.float32)
        masked = jnp.concatenate(
            [jnp.where(row == t * seqs + s, b, 0.0) for t in range(props)], axis=1).astype(jnp.bfloat16)
        x = xdt_ref[:, g * per * size : (g + 1) * per * size]
        outer = dot(x, masked, TN)
        for h in range(per):
            head = g * per + h
            now = first[head]
            for t in range(props):
                now = a_smem[t * seqs + s, head] * now + outer[
                    h * size : (h + 1) * size, t * state : (t + 1) * state]
                out_ref[0, t + 1, head] = now


def local(
    hidden, input_gain, x_weight, z_weight, bc_weight, dt_weight, x_kernel, bc_kernel,
    dt_bias, decay_log, skip_scale, output_gain, output_weight, saved_states,
    x_history, bc_history, accepted,
):
    heads = dt_bias.shape[0]
    seqs, slots, _, size, state = saved_states.shape
    hist = x_history.shape[1]
    inner, bcw = x_weight.shape[1], bc_weight.shape[1]
    n_kv, n_tp = lax.axis_size("kv"), lax.axis_size("tp")
    rows = hidden.shape[0] // n_tp
    n_col = output_weight.shape[1]
    widened = hidden.astype(jnp.float32)
    squares = jnp.sum(widened * widened, axis=1, keepdims=True)
    entry = (widened * input_gain.astype(jnp.float32)).astype(jnp.bfloat16)
    weights = jnp.concatenate([x_weight, z_weight, bc_weight, dt_weight], axis=1)
    product = jnp.dot(entry, weights, preferred_element_type=jnp.float32).astype(jnp.bfloat16)
    fill = jnp.broadcast_to(squares.astype(jnp.bfloat16), (hidden.shape[0], 128 - heads))
    projected = lax.psum_scatter(
        jnp.concatenate([product, fill], axis=1), "tp", scatter_dimension=0, tiled=True)

    params = jnp.pad(jnp.stack([dt_bias, decay_log, skip_scale]), ((0, 5), (0, 128 - heads)))
    vmem = pl.BlockSpec(memory_space=pltpu.VMEM)
    anym = pl.BlockSpec(memory_space=pl.ANY)
    smem = pl.BlockSpec(memory_space=pltpu.SMEM)
    block = n_col // n_kv
    part, xw, bcw_out, xdt, b, a = pl.pallas_call(
        functools.partial(mix_kernel, hidden.shape[1] * n_tp, inner * n_kv, n_kv),
        out_shape=(
            jax.ShapeDtypeStruct((n_kv, rows, block + 128), jnp.bfloat16),
            jax.ShapeDtypeStruct((hist, seqs, inner), jnp.bfloat16),
            jax.ShapeDtypeStruct((hist, seqs, bcw), jnp.bfloat16),
            jax.ShapeDtypeStruct((rows, inner), jnp.bfloat16),
            jax.ShapeDtypeStruct((rows, bcw // 2), jnp.bfloat16),
            jax.ShapeDtypeStruct((rows, 128), jnp.float32),
        ),
        in_specs=[smem] + [vmem] * 8 + [anym] * 2,
        out_specs=[vmem] * 6,
        scratch_shapes=[
            pltpu.VMEM((seqs, heads, size, state), jnp.float32),
            pltpu.VMEM((n_kv, inner, block), jnp.bfloat16),
            pltpu.SemaphoreType.DMA((seqs,)),
            pltpu.SemaphoreType.DMA((n_kv,)),
        ],
        compiler_params=pltpu.CompilerParams(vmem_limit_bytes=40 << 20),
        cost_estimate=pl.CostEstimate(
            flops=2 * rows * inner * n_col, bytes_accessed=14 << 20, transcendentals=0),
        name="mix",
    )(
        accepted, accepted[:, None], projected,
        x_history.transpose(1, 0, 2), bc_history.transpose(1, 0, 2),
        x_kernel, bc_kernel, params, output_gain[None, :], saved_states, output_weight,
    )
    summed = lax.psum_scatter(part, "kv", scatter_dimension=0, tiled=True)[0]

    new_states = pl.pallas_call(
        state_kernel,
        out_shape=jax.ShapeDtypeStruct(saved_states.shape, jnp.float32),
        grid_spec=pltpu.PrefetchScalarGridSpec(
            num_scalar_prefetch=1,
            grid=(seqs,),
            in_specs=[
                smem,
                pl.BlockSpec((rows, inner), lambda s, acc: (0, 0)),
                pl.BlockSpec((rows, bcw // 2), lambda s, acc: (0, 0)),
                pl.BlockSpec((1, 1, heads, size, state), lambda s, acc: (s, acc[s], 0, 0, 0)),
            ],
            out_specs=pl.BlockSpec((1, slots, heads, size, state), lambda s, acc: (s, 0, 0, 0, 0)),
        ),
        compiler_params=pltpu.CompilerParams(vmem_limit_bytes=24 << 20),
        cost_estimate=pl.CostEstimate(
            flops=2 * saved_states.size, bytes_accessed=6 * saved_states.size, transcendentals=0),
        name="states",
    )(accepted, a, xdt, b, saved_states)

    norm = lax.rsqrt(summed[:, block : block + 1].astype(jnp.float32) / (inner * n_kv) + EPSILON)
    mixed = (norm * summed[:, :block].astype(jnp.float32)).astype(jnp.bfloat16)
    return (mixed, new_states, xw.transpose(1, 0, 2), bcw_out.transpose(1, 0, 2))


def fits(mesh):
    inner = INNER // mesh.shape["kv"]
    return inner % 1024 == 0 and mesh.shape["kv"] > 1


def solution(mesh):
    in_specs = (
        P(None, "tp"),
        P("tp"),
        P("tp", "kv"),
        P("tp", "kv"),
        P("tp", "kv"),
        P("tp", "kv"),
        P(None, "kv"),
        P(None, "kv"),
        P("kv"),
        P("kv"),
        P("kv"),
        P("kv"),
        P("kv", None),
        P("tp", None, "kv", None, None),
        P("tp", None, "kv"),
        P("tp", None, "kv"),
        P("tp"),
    )
    out_specs = (
        P("tp", "kv"),
        P("tp", None, "kv", None, None),
        P("tp", None, "kv"),
        P("tp", None, "kv"),
    )
    body = local if fits(mesh) else local_general
    return jax.shard_map(body, mesh=mesh, in_specs=in_specs, out_specs=out_specs, check_vma=False)
```

```python
import jax
import jax.numpy as jnp
import functools

from jax import lax
from jax.experimental import pallas as pl
from jax.experimental.pallas import tpu as pltpu
from jax.sharding import PartitionSpec as P

D = 4096
PROPS = 4
INNER = 8192


EPSILON = 1e-05


def partner_2(block, axis, stride):
    count = lax.axis_size(axis)
    route = []
    for low in range(count):
        high = low | 1 << stride
        if high != low and high < count:
            route += [(low, high), (high, low)]
    return lax.ppermute(block, axis, route)


def take_window(history, accepted, fresh_rows):
    history_len = history.shape[1] - fresh_rows.shape[1]
    indices = accepted[:, None] + jnp.arange(history_len, dtype=jnp.int32)[None, :]
    kept_rows = jnp.take_along_axis(history, indices[:, :, None], axis=1)
    return jnp.concatenate([kept_rows, fresh_rows], axis=1)


def conv_silu(window, kernel):
    length = window.shape[1] - kernel.shape[0] + 1
    running = window[:, 0:length].astype(jnp.float32) * kernel[0].astype(jnp.float32)
    for offset in range(1, kernel.shape[0]):
        running = running + window[:, offset : offset + length].astype(jnp.float32) * kernel[
            offset
        ].astype(jnp.float32)
    return jax.nn.silu(running)


def ssd_block(x_conv, step_size, decay_rate, b_terms, c_terms, first_state, skip_scale):
    cumulated = jnp.cumsum(-decay_rate * step_size, axis=1)
    length = x_conv.shape[1]
    indices = jnp.arange(length)
    causal = indices[:, None] >= indices[None, :]
    gaps = cumulated[:, :, None, :] - cumulated[:, None, :, :]
    weights = jnp.exp(jnp.where(causal[None, :, :, None], gaps, -jnp.inf))
    inputs = x_conv * step_size[..., None]
    outer_prod = jnp.einsum("srhp,srhn->srhpn", inputs, b_terms)
    states = jnp.exp(cumulated)[..., None, None] * first_state[:, None] + jnp.einsum(
        "strh,srhpn->sthpn", weights, outer_prod
    )
    output = jnp.einsum("sthn,sthpn->sthp", c_terms, states) + skip_scale[:, None] * x_conv
    return (output, states)


def local_general(
    hidden,
    input_gain,
    x_weight,
    z_weight,
    bc_weight,
    dt_weight,
    x_kernel,
    bc_kernel,
    dt_bias,
    decay_log,
    skip_scale,
    output_gain,
    output_weight,
    saved_states,
    x_history,
    bc_history,
    accepted,
):
    heads_here = dt_bias.shape[0]
    head_size = x_weight.shape[1] // heads_here
    state_size = saved_states.shape[4]
    seqs_here = accepted.shape[0]
    rows_here = hidden.shape[0] // lax.axis_size("tp")
    inner_here = x_weight.shape[1]
    bc_here = bc_weight.shape[1]
    widened = hidden.astype(jnp.float32)
    squares = lax.psum(jnp.sum(widened * widened, axis=1), "tp")
    normed = (
        widened * lax.rsqrt(squares[:, None] / D + EPSILON) * input_gain.astype(jnp.float32)
    ).astype(jnp.bfloat16)
    weights = jnp.concatenate([x_weight, z_weight, bc_weight, dt_weight], axis=1)
    product = jnp.dot(normed, weights, preferred_element_type=jnp.float32)
    projected = lax.psum_scatter(
        lax.optimization_barrier(product.astype(jnp.bfloat16))
        .astype(jnp.float32)
        .astype(jnp.bfloat16),
        "tp",
        scatter_dimension=0,
        tiled=True,
    )
    x_fresh = projected[:, :inner_here]
    z_fresh = projected[:, inner_here : 2 * inner_here]
    bc_fresh = projected[:, 2 * inner_here : 2 * inner_here + bc_here]
    dt_fresh = projected[:, 2 * inner_here + bc_here :]
    x_window = take_window(x_history, accepted, x_fresh.reshape(seqs_here, PROPS, inner_here))
    bc_window = take_window(bc_history, accepted, bc_fresh.reshape(seqs_here, PROPS, bc_here))
    x_conv = conv_silu(x_window, x_kernel).reshape(seqs_here, PROPS, heads_here, head_size)
    bc_conv = conv_silu(bc_window, bc_kernel)
    spread = max(4 // heads_here, 1)
    position = lax.axis_index("kv")
    for level in range(spread.bit_length() - 1):
        partner = partner_2(bc_conv, "kv", level)
        low_half = position // 2**level % 2 == 0
        bc_conv = jnp.where(
            low_half,
            jnp.concatenate([bc_conv, partner], axis=2),
            jnp.concatenate([partner, bc_conv], axis=2),
        )
    groups_here = bc_conv.shape[2] // (2 * state_size)
    paired = bc_conv.reshape(seqs_here, PROPS, groups_here, 2, state_size)
    per_group = heads_here // groups_here
    b_terms = jnp.repeat(paired[:, :, :, 0], per_group, axis=2)
    c_terms = jnp.repeat(paired[:, :, :, 1], per_group, axis=2)
    step_size = jax.nn.softplus(
        dt_fresh.astype(jnp.float32).reshape(seqs_here, PROPS, heads_here) + dt_bias
    )
    first_state = jnp.take_along_axis(saved_states, accepted[:, None, None, None, None], axis=1)[
        :, 0
    ]
    output, states = ssd_block(
        x_conv, step_size, jnp.exp(decay_log), b_terms, c_terms, first_state, skip_scale
    )
    new_states = jnp.concatenate([first_state[:, None], states], axis=1)
    gate_values = z_fresh.astype(jnp.float32).reshape(seqs_here, PROPS, heads_here, head_size)
    gated = (output * jax.nn.silu(gate_values)).reshape(rows_here, inner_here)
    square_sum = jnp.sum(gated * gated, axis=1)
    scaled = (gated * output_gain.astype(jnp.float32)).astype(jnp.bfloat16)
    partial_value = jnp.dot(scaled, output_weight, preferred_element_type=jnp.float32)
    total_squares = lax.psum(square_sum, "kv")
    summed = lax.psum_scatter(partial_value, "kv", scatter_dimension=1, tiled=True)
    mixed = (lax.rsqrt(total_squares / INNER + EPSILON)[:, None] * summed).astype(jnp.bfloat16)
    return (mixed, new_states, x_window, bc_window)


NN = (((1,), (0,)), ((), ()))
NT = (((1,), (1,)), ((), ()))
TN = (((0,), (0,)), ((), ()))


def dot(a, b, dims=NN, **kw):
    return lax.dot_general(a, b, dims, preferred_element_type=jnp.float32, **kw)


def silu(v):
    return v / (1.0 + jnp.exp(-v))


def softplus(v):
    return jnp.maximum(v, 0.0) + jnp.log(1.0 + jnp.exp(-jnp.abs(v)))


def mix_kernel(
    features, channels, n_out,
    acc_smem, bias_smem, decay_smem, skip_smem, proj_ref, xh_ref, bch_ref, xk_ref, bck_ref, gain_ref,
    saved_ref, w_ref,
    part_ref, xw_ref, bcw_ref, xdt_ref, b_ref, a_ref,
    s0_buf, w_buf, s0_sem, w_sem,
):
    seqs = acc_smem.shape[0]
    props = proj_ref.shape[0] // seqs
    rows = seqs * props
    inner = xh_ref.shape[2]
    bcw = bch_ref.shape[2]
    heads, size, state = s0_buf.shape[1:]
    groups = bcw // (2 * state)
    per = heads // groups
    span = per * size

    def s0_copy(s):
        return pltpu.make_async_copy(
            saved_ref.at[s, acc_smem[s]], s0_buf.at[s], s0_sem.at[s])

    for s in range(seqs):
        s0_copy(s).start()
    block = w_ref.shape[1] // n_out
    w_copies = [
        pltpu.make_async_copy(
            w_ref.at[:, pl.ds(i * block, block)], w_buf.at[i], w_sem.at[i])
        for i in range(n_out)
    ]
    for copy in w_copies:
        copy.start()

    ri = lax.broadcasted_iota(jnp.int32, (rows, rows), 0)
    ci = lax.broadcasted_iota(jnp.int32, (rows, rows), 1)
    to_steps = ((ri % seqs) * props + ri // seqs == ci).astype(jnp.float32).astype(jnp.bfloat16)
    back = ((ci % seqs) * props + ci // seqs == ri).astype(jnp.float32).astype(jnp.bfloat16)

    dt_at = 2 * inner + bcw
    last = proj_ref.shape[1]
    squares = proj_ref[:, last - 128 :].astype(jnp.float32)[:, 127:128]
    scale = lax.rsqrt(squares / features + EPSILON)

    def fresh(lo, hi):
        v = (proj_ref[:, lo:hi].astype(jnp.float32) * scale).astype(jnp.bfloat16)
        return dot(to_steps, v)

    def step(v, t):
        return v[t * seqs : (t + 1) * seqs]

    seq_at = lax.broadcasted_iota(jnp.int32, (seqs, inner), 0)
    acc = jnp.zeros((seqs, inner), jnp.int32)
    for s in range(seqs):
        acc = jnp.where(seq_at == s, acc_smem[s], acc)

    def window(hist_ref, rows_fresh, out_ref):
        kept = hist_ref.shape[0] - props
        hist = [hist_ref[m].astype(jnp.float32) for m in range(hist_ref.shape[0])]
        win = []
        for k in range(kept):
            v = hist[k]
            for j in range(1, props + 1):
                v = jnp.where(acc[:, :1] == j, hist[j + k], v)
            win.append(v)
        win += [step(rows_fresh, t) for t in range(props)]
        for m, v in enumerate(win):
            out_ref[m] = v.astype(jnp.bfloat16)
        return win

    def conv(win, kernel_ref):
        taps = [kernel_ref[j : j + 1].astype(jnp.float32) for j in range(kernel_ref.shape[0])]
        out = []
        for t in range(props):
            v = win[t] * taps[0]
            for j in range(1, len(taps)):
                v = v + win[t + j] * taps[j]
            out.append(silu(v))
        return out

    bc = conv(window(bch_ref, fresh(2 * inner, dt_at), bcw_ref), bck_ref)
    b_all = jnp.concatenate(
        [jnp.concatenate([v[:, 2 * g * state : (2 * g + 1) * state] for g in range(groups)], axis=1) for v in bc], axis=0)
    c_all = jnp.concatenate(
        [jnp.concatenate([v[:, (2 * g + 1) * state : (2 * g + 2) * state] for g in range(groups)], axis=1) for v in bc], axis=0)
    b_ref[...] = b_all.astype(jnp.bfloat16)
    c_low = c_all.astype(jnp.bfloat16)
    xc = conv(window(xh_ref, fresh(0, inner), xw_ref), xk_ref)

    dt_raw = fresh(dt_at, last)
    eh = lax.broadcasted_iota(jnp.int32, (128, inner), 0)
    ec = lax.broadcasted_iota(jnp.int32, (128, inner), 1)
    expand = (eh == ec // size).astype(jnp.float32)
    lane_at = lax.broadcasted_iota(jnp.int32, (8, 128), 1)
    row_at = lax.broadcasted_iota(jnp.int32, (8, 128), 0)
    par = jnp.zeros((8, 128), jnp.float32)
    for i, smem in enumerate((bias_smem, decay_smem, skip_smem)):
        for h in range(heads):
            par = jnp.where((row_at == i) & (lane_at == h), smem[h], par)
    wide = dot(par, expand, precision=lax.Precision.HIGHEST)
    dtw = dot(dt_raw.astype(jnp.bfloat16), expand.astype(jnp.bfloat16))
    lane = lax.broadcasted_iota(jnp.int32, (rows, 128), 1)
    raw = jnp.where(lane < heads, dt_raw, 0.0)
    a_ref[...] = jnp.exp(-jnp.exp(par[1:2]) * softplus(raw + par[0:1]))
    bias, rate, skip = wide[0:1], jnp.exp(wide[1:2]), wide[2:3]
    sizes = [softplus(step(dtw, t) + bias) for t in range(props)]
    xdt = [xc[t] * sizes[t] for t in range(props)]
    xdt_ref[...] = jnp.concatenate(xdt, axis=0).astype(jnp.bfloat16)

    row = lax.broadcasted_iota(jnp.int32, (rows, span), 0)
    carried = [jnp.zeros((rows, span), jnp.float32) for _ in range(groups)]
    for s in range(seqs):
        s0_copy(s).wait()
        for g in range(groups):
            s0 = s0_buf[s, g * per : (g + 1) * per].reshape(span, state).astype(jnp.bfloat16)
            got = dot(c_low[:, g * state : (g + 1) * state], s0, NT)
            carried[g] = jnp.where(row % seqs == s, got, carried[g])
    carried = jnp.concatenate(carried, axis=1)

    decays = [-rate * v for v in sizes]
    gated, sums = [], []
    zs = fresh(inner, 2 * inner)
    gain = gain_ref[...].astype(jnp.float32).reshape(1, inner)
    for t in range(props):
        total = decays[t]
        out = skip * xc[t]
        ct = step(c_all, t)
        for r in range(t, -1, -1):
            br = step(b_all, r)
            prod = ct * br
            pair = jnp.concatenate(
                [jnp.broadcast_to(
                    jnp.sum(prod[:, g * state : (g + 1) * state], axis=1, keepdims=True),
                    (seqs, span)) for g in range(groups)], axis=1)
            if r == t:
                out = out + pair * xdt[r]
            else:
                out = out + jnp.exp(total) * pair * xdt[r]
                total = total + decays[r]
        out = out + jnp.exp(total) * step(carried, t)
        v = out * silu(step(zs, t))
        gated.append((v * gain).astype(jnp.bfloat16))
        sums.append(jnp.broadcast_to(jnp.sum(v * v, axis=1, keepdims=True), (seqs, 128)))
    scaled = dot(back, jnp.concatenate(gated, axis=0)).astype(jnp.bfloat16)
    sums = jnp.concatenate(sums, axis=0)
    high = sums.astype(jnp.bfloat16)
    low = (sums - high.astype(jnp.float32)).astype(jnp.bfloat16)
    sums = dot(back, high) + dot(back, low)
    for i in range(n_out):
        w_copies[i].wait()
        part_ref[i, :, :block] = dot(scaled, w_buf[i]).astype(part_ref.dtype)
        part_ref[i, :, block:] = sums.astype(part_ref.dtype)


def state_kernel(acc_smem, a_smem, xdt_ref, b_ref, s0_ref, out_ref):
    s = pl.program_id(0)
    seqs = acc_smem.shape[0]
    rows = xdt_ref.shape[0]
    props = rows // seqs
    heads, size, state = s0_ref.shape[2:]
    groups = b_ref.shape[1] // state
    per = heads // groups
    row = lax.broadcasted_iota(jnp.int32, (rows, state), 0)
    first = s0_ref[0, 0]
    out_ref[0, 0] = first
    for g in range(groups):
        b = b_ref[:, g * state : (g + 1) * state].astype(jnp.float32)
        masked = jnp.concatenate(
            [jnp.where(row == t * seqs + s, b, 0.0) for t in range(props)], axis=1).astype(jnp.bfloat16)
        x = xdt_ref[:, g * per * size : (g + 1) * per * size]
        outer = dot(x, masked, TN)
        for h in range(per):
            head = g * per + h
            now = first[head]
            for t in range(props):
                now = a_smem[t * seqs + s, head] * now + outer[
                    h * size : (h + 1) * size, t * state : (t + 1) * state]
                out_ref[0, t + 1, head] = now


def exchange(axis, blocks_ref, slots, send_sems, recv_sems):
    count = blocks_ref.shape[0]
    me = lax.axis_index(axis)
    barrier = pltpu.get_barrier_semaphore()
    for d in range(1, count):
        pl.semaphore_signal(
            barrier, inc=1, device_id={axis: lax.rem(me + d, count)}, device_id_type=pl.DeviceIdType.MESH)
    pl.semaphore_wait(barrier, count - 1)
    copies = []
    for d in range(1, count):
        peer = lax.rem(me + d, count)
        copies.append(pltpu.make_async_remote_copy(
            src_ref=blocks_ref.at[peer],
            dst_ref=slots.at[d - 1],
            send_sem=send_sems.at[d - 1],
            recv_sem=recv_sems.at[d - 1],
            device_id={axis: peer},
            device_id_type=pl.DeviceIdType.MESH,
        ))
    for copy in copies:
        copy.start()
    total = blocks_ref[me].astype(jnp.float32)
    for d, copy in enumerate(copies):
        copy.wait_recv()
        total = total + slots[d].astype(jnp.float32)
    for copy in copies:
        copy.wait_send()
    return total


def entry_kernel(blocks_ref, out_ref, *scratch):
    out_ref[...] = exchange("tp", blocks_ref, *scratch)


def exit_kernel(channels, blocks_ref, out_ref, *scratch):
    total = exchange("kv", blocks_ref, *scratch)
    width = out_ref.shape[1]
    norm = lax.rsqrt(total[:, width : width + 1] / channels + EPSILON)
    out_ref[...] = (norm * total[:, :width]).astype(out_ref.dtype)


def exchange_call(body, name, number, blocks, out_shape):
    count = blocks.shape[0]
    return pl.pallas_call(
        body,
        out_shape=out_shape,
        in_specs=[pl.BlockSpec(memory_space=pltpu.VMEM)],
        out_specs=pl.BlockSpec(memory_space=pltpu.VMEM),
        scratch_shapes=[
            pltpu.VMEM((count - 1,) + blocks.shape[1:], blocks.dtype),
            pltpu.SemaphoreType.DMA((count - 1,)),
            pltpu.SemaphoreType.DMA((count - 1,)),
        ],
        compiler_params=pltpu.CompilerParams(collective_id=number, has_side_effects=True),
        name=name,
    )(blocks)


def local(
    hidden, input_gain, x_weight, z_weight, bc_weight, dt_weight, x_kernel, bc_kernel,
    dt_bias, decay_log, skip_scale, output_gain, output_weight, saved_states,
    x_history, bc_history, accepted,
):
    heads = dt_bias.shape[0]
    seqs, slots, _, size, state = saved_states.shape
    hist = x_history.shape[1]
    inner, bcw = x_weight.shape[1], bc_weight.shape[1]
    n_kv, n_tp = lax.axis_size("kv"), lax.axis_size("tp")
    rows = hidden.shape[0] // n_tp
    n_col = output_weight.shape[1]
    widened = hidden.astype(jnp.float32)
    squares = jnp.sum(widened * widened, axis=1, keepdims=True)
    entry = (widened * input_gain.astype(jnp.float32)).astype(jnp.bfloat16)
    weights = jnp.concatenate([x_weight, z_weight, bc_weight, dt_weight], axis=1)
    product = jnp.dot(entry, weights, preferred_element_type=jnp.float32).astype(jnp.bfloat16)
    fill = jnp.broadcast_to(squares.astype(jnp.bfloat16), (hidden.shape[0], 128 - heads))
    projected = exchange_call(
        entry_kernel, "entry_exchange", 0,
        jnp.concatenate([product, fill], axis=1).reshape(n_tp, rows, -1),
        jax.ShapeDtypeStruct((rows, product.shape[1] + 128 - heads), jnp.float32))

    vmem = pl.BlockSpec(memory_space=pltpu.VMEM)
    anym = pl.BlockSpec(memory_space=pl.ANY)
    smem = pl.BlockSpec(memory_space=pltpu.SMEM)
    block = n_col // n_kv
    part, xw, bcw_out, xdt, b, a = pl.pallas_call(
        functools.partial(mix_kernel, hidden.shape[1] * n_tp, inner * n_kv, n_kv),
        out_shape=(
            jax.ShapeDtypeStruct((n_kv, rows, block + 128), jnp.bfloat16),
            jax.ShapeDtypeStruct((hist, seqs, inner), jnp.bfloat16),
            jax.ShapeDtypeStruct((hist, seqs, bcw), jnp.bfloat16),
            jax.ShapeDtypeStruct((rows, inner), jnp.bfloat16),
            jax.ShapeDtypeStruct((rows, bcw // 2), jnp.bfloat16),
            jax.ShapeDtypeStruct((rows, 128), jnp.float32),
        ),
        in_specs=[smem] * 4 + [vmem] * 6 + [anym] * 2,
        out_specs=[vmem] * 6,
        scratch_shapes=[
            pltpu.VMEM((seqs, heads, size, state), jnp.float32),
            pltpu.VMEM((n_kv, inner, block), jnp.bfloat16),
            pltpu.SemaphoreType.DMA((seqs,)),
            pltpu.SemaphoreType.DMA((n_kv,)),
        ],
        compiler_params=pltpu.CompilerParams(vmem_limit_bytes=60 << 20),
        cost_estimate=pl.CostEstimate(
            flops=2 * rows * inner * n_col, bytes_accessed=14 << 20, transcendentals=0),
        name="mix",
    )(
        accepted, dt_bias, decay_log, skip_scale, projected,
        x_history.transpose(1, 0, 2), bc_history.transpose(1, 0, 2),
        x_kernel, bc_kernel, output_gain, saved_states, output_weight,
    )
    mixed = exchange_call(
        functools.partial(exit_kernel, inner * n_kv), "exit_exchange", 1, part,
        jax.ShapeDtypeStruct((rows, block), jnp.bfloat16))

    new_states = pl.pallas_call(
        state_kernel,
        out_shape=jax.ShapeDtypeStruct(saved_states.shape, jnp.float32),
        grid_spec=pltpu.PrefetchScalarGridSpec(
            num_scalar_prefetch=1,
            grid=(seqs,),
            in_specs=[
                smem,
                pl.BlockSpec((rows, inner), lambda s, acc: (0, 0)),
                pl.BlockSpec((rows, bcw // 2), lambda s, acc: (0, 0)),
                pl.BlockSpec((1, 1, heads, size, state), lambda s, acc: (s, acc[s], 0, 0, 0)),
            ],
            out_specs=pl.BlockSpec((1, slots, heads, size, state), lambda s, acc: (s, 0, 0, 0, 0)),
        ),
        compiler_params=pltpu.CompilerParams(vmem_limit_bytes=60 << 20),
        cost_estimate=pl.CostEstimate(
            flops=2 * saved_states.size, bytes_accessed=6 * saved_states.size, transcendentals=0),
        name="states",
    )(accepted, a, xdt, b, saved_states)

    return (mixed, new_states, xw.transpose(1, 0, 2), bcw_out.transpose(1, 0, 2))


def fits(mesh):
    inner = INNER // mesh.shape["kv"]
    return inner % 1024 == 0 and mesh.shape["kv"] > 1


def solution(mesh):
    in_specs = (
        P(None, "tp"),
        P("tp"),
        P("tp", "kv"),
        P("tp", "kv"),
        P("tp", "kv"),
        P("tp", "kv"),
        P(None, "kv"),
        P(None, "kv"),
        P("kv"),
        P("kv"),
        P("kv"),
        P("kv"),
        P("kv", None),
        P("tp", None, "kv", None, None),
        P("tp", None, "kv"),
        P("tp", None, "kv"),
        P("tp"),
    )
    out_specs = (
        P("tp", "kv"),
        P("tp", None, "kv", None, None),
        P("tp", None, "kv"),
        P("tp", None, "kv"),
    )
    body = local if fits(mesh) else local_general
    return jax.shard_map(body, mesh=mesh, in_specs=in_specs, out_specs=out_specs, check_vma=False)
```
